32 devices in a mesh: sp: 8 (over z, y), tp: 4 (over x, core).
Axes of the slice: x: 2, y: 2, z: 4, core: 2. Of those that a mesh axis runs over, the one named last changes fastest.
Arguments:
- gate_in: bfloat16 [4096, 2048], P('sp', 'tp'), may hold values from -6 to 6
- value_in: bfloat16 [4096, 2048], P('sp', 'tp'), may hold values from -6 to 6
- gate_out: bfloat16 [4096, 2048], P('sp', 'tp'), may hold values from -6 to 6
- conv_taps: float32 [3, 2048], P(None, 'tp'), may hold values from -3.5 to 3.5
- proj_weight: bfloat16 [2048, 2048], P('tp'), may hold values from -0.125 to 0.125
- residual: bfloat16 [4096, 2048], P(('sp', 'tp')), may hold values from -6 to 6
- norm_gain: float32 [2048], replicated, may hold values from 0.1 to 1.9
- routes: int32 [4096, 2], P('sp'), may hold values from 0 to 7, all different within a row; in each aligned block of 128 rows (0 to 127, 128 to 255, ...) at most 64 rows name the same one
- route_weight: float32 [4096, 2], P('sp'), may hold values from 0.1 to 0.9
- expert_gate: bfloat16 [8, 2048, 2048], P('sp', None, 'tp'), may hold values from -0.125 to 0.125
- expert_up: bfloat16 [8, 2048, 2048], P('sp', None, 'tp'), may hold values from -0.125 to 0.125
- expert_down: bfloat16 [8, 2048, 2048], P('sp', 'tp'), may hold values from -0.125 to 0.125
Outputs:
- layer_out: bfloat16 [4096, 2048], P(('sp', 'tp'))
The draws below stay inside these ranges and needn't reach their ends.
Inputs may be any that keep to these rules, and one draw needn't show every extreme that they name: `routes`: A token's 2 experts differ. In each aligned block of 128 tokens no expert is named by more than 64 tokens, a bound that some block reaches.
All inputs are finite; a program needn't handle non-finite values.
Results may differ from the reference program's by a relative error of at most 0.012.
Values may be sent and summed in bfloat16 or wider, within the bound.
A program may use at most 128 MiB of HBM per device.

```python
import math
import jax
import jax.numpy as jnp
import numpy as np
from jax import lax

D = 2048
FE = 2048
TOP = 2
TAPS = 3
TOK_DEV = 512
TOKQ = 128
EXPERTS = 8
CAPQ = 64
TOKENS = 4096
N_SP = 8
N_TP = 4


def levels(key, shape, shards, least, largest):
    gain, own = 1.0, jax.random.fold_in(key, 6)
    for position, blocks in shards:
        heights = jnp.exp(jax.random.uniform(jax.random.fold_in(own, position), (blocks,), jnp.float32, least / len(shards), largest / len(shards)))
        gain = gain * jnp.repeat(heights, shape[position] // blocks).reshape([-1 if axis == position else 1 for axis in range(len(shape))])
    return gain


def routed_block(key, own, number, rows, count, top, bound, lean):
    sequence = jax.random.permutation(key, count)
    heavy_load, ordinary = shares(count, rows * top, bound, lean, True), shares(count, rows * top, bound, lean, False)
    places = jnp.arange(count)

    def named(lengths, rotation):
        used = int((lengths > 0).sum())
        fixed = max(1, used // 4)
        moved = fixed + (places - fixed + rotation * (used - fixed)) % max(1, count - fixed)
        return jnp.zeros((count,), jnp.int32).at[sequence[jnp.where(places < fixed, places, moved)]].set(jnp.asarray(lengths, jnp.int32))

    lengths = jnp.where(number % 4 == 0, named(heavy_load, number // 4), named(ordinary, number - number // 4 - 1))
    mixed = jax.random.permutation(jax.random.fold_in(own, 3), count)
    giver, sink = mixed[0:count // 2 * 2:2], mixed[1:count // 2 * 2:2]
    slack = jnp.minimum(lengths[giver] - 1, bound - lengths[sink]) // 2
    slack = jnp.where((giver == sequence[0]) | (sink == sequence[0]) | (lengths[sink] == 0), 0, jnp.maximum(slack, 0))
    moved = jax.random.randint(jax.random.fold_in(own, 4), (count // 2,), 0, 1 << 20) % (slack + 1)
    lengths = lengths.at[giver].add(-moved).at[sink].add(moved)
    items = jnp.searchsorted(jnp.cumsum(lengths), jnp.arange(rows * top), side="right").astype(jnp.int32)
    table = items.reshape(top, rows).T
    table = table[jax.random.permutation(jax.random.fold_in(own, 1), rows)]
    rotation = jax.random.randint(jax.random.fold_in(own, 2), (rows, 1), 0, top)
    return jnp.take_along_axis(table, (jnp.arange(top)[None, :] + rotation) % top, axis=1)


def shares(count, total, most, slope, full):
    loads = [(1 << 20) // math.isqrt(rank ** slope) + 1 for rank in range(1, count + 1)]
    largest = most if full else min(most, max(-(-total // count), total * loads[0] // sum(loads)))
    least = 1 if total - largest >= count - 1 else 0
    given, rest = [largest] + [least] * (count - 1), total - largest - least * (count - 1)
    while rest > 0:
        candidates = [i for i in range(1, count) if given[i] < largest] or [i for i in range(1, count) if given[i] < most]
        pool, left = sum([loads[i] for i in candidates]), rest
        for i in candidates:
            extra = min(most - given[i], max(1, left * loads[i] // pool), rest)
            given[i] = given[i] + extra
            rest = rest - extra
    return np.array(given)


def bell_draw(key, extent, spread, reach, cuts=(), kind=jnp.bfloat16):
    array = jax.random.normal(key, extent, jnp.float32) * spread
    if len(cuts) > 0:
        array = levels(key, extent, cuts, -0.22, 0.18) * array
    return jnp.clip(array, min=-reach, max=reach).astype(kind)


def setup_inputs(seed: int = 0) -> dict:
    key_list = jax.random.split(jax.random.key(seed), 13)
    gate_in = bell_draw(key_list[0], (TOKENS, D), 1.0, 6.0, ((0, 8), (1, 4)))
    value_in = bell_draw(key_list[1], (TOKENS, D), 1.0, 6.0, ((0, 8), (1, 4)))
    gate_out = bell_draw(key_list[2], (TOKENS, D), 1.0, 6.0, ((0, 8), (1, 4)))
    conv_taps = bell_draw(key_list[3], (TAPS, D), TAPS ** -0.5, 3.5, ((1, 4),), jnp.float32)
    proj_weight = bell_draw(key_list[4], (D, D), D ** -0.5, 0.125, ((0, 4),))
    residual = bell_draw(key_list[5], (TOKENS, D), 1.0, 6.0, ((0, 32),))
    norm_gain = jnp.clip(1.0 + 0.18 * jax.random.normal(key_list[6], (D,), jnp.float32), 0.1, 1.9)
    routes_keys = jax.random.split(jax.random.fold_in(key_list[7], 1), TOKENS // TOKQ)
    routes_turns = jax.random.permutation(jax.random.fold_in(key_list[7], 3), TOKENS // TOKQ)
    routes = jax.vmap(lambda own, number: routed_block(jax.random.fold_in(key_list[7], 2), own, number, TOKQ, EXPERTS, TOP, CAPQ, 2))(routes_keys, routes_turns).reshape((TOKENS, TOP))
    route_weight = jnp.clip(0.1 + 0.79999997 * jax.random.uniform(key_list[8], (TOKENS, TOP), jnp.float32) ** levels(key_list[8], (TOKENS, TOP), ((0, 8),), -0.2, 0.2), 0.1, 0.9)
    expert_gate = bell_draw(key_list[9], (EXPERTS, D, FE), D ** -0.5, 0.125, ((0, 8), (2, 4)))
    expert_up = bell_draw(key_list[10], (EXPERTS, D, FE), D ** -0.5, 0.125, ((0, 8), (2, 4)))
    expert_down = bell_draw(key_list[11], (EXPERTS, FE, D), FE ** -0.5, 0.125, ((0, 8), (1, 4)))
    return dict(gate_in=gate_in, value_in=value_in, gate_out=gate_out, conv_taps=conv_taps, proj_weight=proj_weight, residual=residual, norm_gain=norm_gain, routes=routes, route_weight=route_weight, expert_gate=expert_gate, expert_up=expert_up, expert_down=expert_down)


def rounded(values):
    return lax.optimization_barrier(values.astype(jnp.bfloat16)).astype(jnp.float32)

def slot_numbers(route_ids, block_rows, expert_count):
    block_count = route_ids.shape[0] // block_rows
    flat_ids = route_ids.reshape(block_count, block_rows * route_ids.shape[1])
    one_hot = (flat_ids[:, :, None] == jnp.arange(expert_count, dtype=jnp.int32)[None, None, :]).astype(jnp.int32)
    before = jnp.cumsum(one_hot, axis=1) - one_hot
    return lax.optimization_barrier(jnp.sum(before * one_hot, axis=2)).reshape(route_ids.shape).astype(jnp.int32)

def normalize(hidden_rows, norm_gain):
    inverse = lax.rsqrt(lax.optimization_barrier(jnp.mean(hidden_rows * hidden_rows, axis=-1, keepdims=True)) + 1e-05)
    return (hidden_rows * inverse * norm_gain.astype(jnp.float32)).astype(jnp.bfloat16)

def mixer_output(gate_in, value_in, gate_out, conv_taps, prior_gate, prior_value):
    product = gate_in.astype(jnp.float32) * value_in.astype(jnp.float32)
    prior_mix = prior_gate.astype(jnp.float32) * prior_value.astype(jnp.float32)
    padded = jnp.concatenate([prior_mix, product], axis=0)
    taps = conv_taps.astype(jnp.float32)
    conv_sum = taps[0] * padded[:-2] + taps[1] * padded[1:-1] + taps[2] * padded[2:]
    return (gate_out.astype(jnp.float32) * conv_sum).astype(jnp.bfloat16)

def reference(gate_in, value_in, gate_out, conv_taps, proj_weight, residual, norm_gain, routes, route_weight, expert_gate, expert_up, expert_down):
    model_width = residual.shape[1]
    zero_rows = jnp.zeros((2, gate_in.shape[1]), jnp.bfloat16)
    mixed_out = mixer_output(gate_in, value_in, gate_out, conv_taps, zero_rows, zero_rows)
    slice_width = model_width // N_TP
    summed = jnp.zeros(residual.shape, jnp.float32)
    for group in range(N_TP):
        lower = group * slice_width
        summed = summed + rounded(jnp.dot(mixed_out[:, lower:lower + slice_width], proj_weight[lower:lower + slice_width], preferred_element_type=jnp.float32))
    hidden_rows = residual.astype(jnp.float32) + summed
    normed = normalize(hidden_rows, norm_gain)
    token_count = residual.shape[0]
    top_count = routes.shape[1]
    slots = slot_numbers(routes, TOKQ, EXPERTS)
    token_ids = jnp.arange(token_count, dtype=jnp.int32)
    source = token_ids // TOK_DEV
    quarter = token_ids % TOK_DEV // TOKQ
    flat_index = ((routes * N_TP + quarter[:, None]) * N_SP + source[:, None]) * CAPQ + slots
    per_expert = N_TP * N_SP * CAPQ
    slot_count = EXPERTS * per_expert
    slot_token = jnp.full((slot_count,), token_count, jnp.int32).at[flat_index.reshape(-1)].set(jnp.repeat(token_ids, top_count))
    slot_weight = jnp.zeros((slot_count,), jnp.float32).at[flat_index.reshape(-1)].set(route_weight.reshape(-1))
    padded_rows = jnp.concatenate([normed, jnp.zeros((1, model_width), jnp.bfloat16)], axis=0)
    hidden_width = expert_gate.shape[2] // N_TP

    def one_expert(total, expert):
        start_row = (expert * per_expert).astype(jnp.int32)
        chosen = lax.dynamic_slice_in_dim(slot_token, start_row, per_expert, 0)
        weights_now = lax.dynamic_slice_in_dim(slot_weight, start_row, per_expert, 0)
        row_block = padded_rows[chosen]
        gate_pre = jnp.dot(row_block, expert_gate[expert], preferred_element_type=jnp.float32)
        up_pre = jnp.dot(row_block, expert_up[expert], preferred_element_type=jnp.float32)
        hidden = (jax.nn.silu(gate_pre) * up_pre).astype(jnp.bfloat16)
        down_weight = expert_down[expert]
        partial_sum = jnp.zeros((per_expert, model_width), jnp.float32)
        for group in range(N_TP):
            lower = group * hidden_width
            partial_sum = partial_sum + rounded(jnp.dot(hidden[:, lower:lower + hidden_width], down_weight[lower:lower + hidden_width], preferred_element_type=jnp.float32))
        expert_rows = rounded(partial_sum)
        total = total.at[chosen].add(weights_now[:, None] * expert_rows)
        return (total, None)
    total, _ = lax.scan(one_expert, jnp.zeros((token_count + 1, model_width), jnp.float32), jnp.arange(EXPERTS, dtype=jnp.int32))
    return (hidden_rows + total[:token_count]).astype(jnp.bfloat16)
```

```python
import functools

import jax
import jax.numpy as jnp
from jax import lax
from jax.experimental import pallas as pl
from jax.experimental.pallas import tpu as pltpu
from jax.sharding import PartitionSpec as P


def passed_along(shard, axis, by):
    size = lax.axis_size(axis)
    pairs = [(i, i + by) for i in range(size) if 0 <= i + by < size]
    return lax.ppermute(shard, axis, pairs)


def rounded(values):
    return lax.optimization_barrier(values.astype(jnp.bfloat16)).astype(jnp.float32)


def slot_numbers(route_ids, block_rows, expert_count):
    block_count = route_ids.shape[0] // block_rows
    flat_ids = route_ids.reshape(block_count, block_rows * route_ids.shape[1])
    one_hot = (
        flat_ids[:, :, None] == jnp.arange(expert_count, dtype=jnp.int32)[None, None, :]
    ).astype(jnp.int32)
    before = jnp.cumsum(one_hot, axis=1) - one_hot
    return jnp.sum(before * one_hot, axis=2).reshape(route_ids.shape)


def normalize(hidden_rows, norm_gain):
    inverse = lax.rsqrt(jnp.mean(hidden_rows * hidden_rows, axis=-1, keepdims=True) + 1e-05)
    return (hidden_rows * inverse * norm_gain).astype(jnp.bfloat16)


def dispatch_rows(normed, flat_pick, slot_count):
    slot_ids = jnp.arange(slot_count, dtype=jnp.int32)
    chosen = jnp.any(flat_pick[None, :, :] == slot_ids[:, None, None], axis=2)
    return jnp.dot(
        chosen.astype(jnp.bfloat16), normed, preferred_element_type=jnp.float32
    ).astype(jnp.bfloat16)


MESH = pl.DeviceIdType.MESH


def expert_kernel(
    n, tp, out_ref, gate_hbm, up_hbm, down_hbm, ret_ref,
    recv, part, mrecv, psum, xrecv, fin, gate_w, up_w, down_w, hid, local_sem, send, got,
):
    s = lax.axis_index("sp")
    t = lax.axis_index("tp")
    mate = t + 1 - 2 * (t % 2)
    across = (t + 2) % tp
    mate_across = (mate + 2) % tp
    cap, width = out_ref.shape[1], out_ref.shape[2]
    units = gate_w.shape[1]
    rows = tp * cap

    weight_copies = [
        pltpu.make_async_copy(src, dst, local_sem.at[i])
        for i, (src, dst) in enumerate(
            [(gate_hbm, gate_w), (up_hbm, up_w), (down_hbm, down_w)]
        )
    ]
    for copy in weight_copies:
        copy.start()

    barrier = pltpu.get_barrier_semaphore()

    @pl.loop(1, n)
    def _(k):
        pl.semaphore_signal(barrier, inc=1, device_id=((s + k) % n, t), device_id_type=MESH)

    for peer in (mate, across):
        pl.semaphore_signal(barrier, inc=1, device_id=(s, peer), device_id_type=MESH)
    pl.semaphore_wait(barrier, n + 1)

    def remote(src, dst, lane, k, device):
        return pltpu.make_async_remote_copy(
            src_ref=src,
            dst_ref=dst,
            send_sem=send.at[lane, k],
            recv_sem=got.at[lane, k],
            device_id=device,
            device_id_type=MESH,
        )

    def outward(k):
        to = (s + k) % n
        return remote(out_ref.at[to], recv.at[k, t], 0, k, (to, t))

    def over(k, block):
        return remote(recv.at[k, block], recv.at[k, block], 1, k, (s, across))

    def pair_own(k, block):
        return remote(recv.at[k, block], recv.at[k, block], 2, k, (s, mate))

    def pair_far(k, block):
        return remote(recv.at[k, block], recv.at[k, block], 3, k, (s, mate))

    def part_near(k):
        return remote(part.at[k, mate], mrecv.at[k, 0], 4, k, (s, mate))

    def part_far(k):
        return remote(part.at[k, mate_across], mrecv.at[k, 1], 5, k, (s, mate))

    def sum_over(k):
        return remote(psum.at[k], xrecv.at[k], 6, k, (s, across))

    def homeward(k):
        return remote(fin.at[k], ret_ref.at[s], 7, k, ((s + n - k) % n, t))

    own = pltpu.make_async_copy(out_ref.at[s], recv.at[0, t], local_sem.at[3])
    own.start()

    @pl.loop(1, n)
    def _(k):
        outward(k).start()

    own.wait()

    def ffn(k):
        def load():
            block = recv[k]
            if cap % 16:
                return block.astype(jnp.float32).reshape(rows, width).astype(jnp.bfloat16)
            return block.reshape(rows, width)

        cols = min(256, units)

        @pl.loop(0, units // cols)
        def _(c):
            at = pl.ds(pl.multiple_of(c * cols, cols), cols)
            x = load()
            gate = jnp.dot(x, gate_w[:, at], preferred_element_type=jnp.float32)
            up = jnp.dot(x, up_w[:, at], preferred_element_type=jnp.float32)
            hid[:, at] = (gate / (1.0 + jnp.exp(-gate)) * up).astype(jnp.bfloat16)

        wide = min(512, width)

        @pl.loop(0, width // wide)
        def _(c):
            at = pl.ds(pl.multiple_of(c * wide, wide), wide)
            y = jnp.dot(hid[...], down_w[:, at], preferred_element_type=jnp.float32)
            part[k, :, :, at] = y.reshape(tp, cap, wide).astype(jnp.bfloat16)

    def wide_sum(*blocks):
        total = blocks[0].astype(jnp.float32)
        for block in blocks[1:]:
            total = total + block.astype(jnp.float32)
        return total

    @pl.loop(0, n + 4)
    def _(i):
        @pl.when(i < n)
        def _():
            @pl.when(i > 0)
            def _():
                outward(i).wait_recv()

            over(i, t).start()
            pair_own(i, t).start()

        @pl.when((i >= 1) & (i < n + 1))
        def _():
            k = i - 1
            over(k, across).wait_recv()
            pair_far(k, across).start()

        @pl.when(i == 2)
        def _():
            for copy in weight_copies:
                copy.wait()

        @pl.when((i >= 2) & (i < n + 2))
        def _():
            k = i - 2
            pair_own(k, mate).wait_recv()
            pair_far(k, mate_across).wait_recv()
            ffn(k)
            part_far(k).start()
            part_near(k).start()

        @pl.when((i >= 3) & (i < n + 3))
        def _():
            k = i - 3
            part_far(k).wait_recv()
            psum[k] = wide_sum(part[k, across], mrecv[k, 1]).astype(jnp.bfloat16)
            sum_over(k).start()

        @pl.when(i >= 4)
        def _():
            k = i - 4
            part_near(k).wait_recv()
            sum_over(k).wait_recv()
            total = wide_sum(part[k, t], mrecv[k, 0], xrecv[k]).astype(jnp.bfloat16)

            @pl.when(k == 0)
            def _():
                ret_ref[s] = total

            @pl.when(k > 0)
            def _():
                fin[k] = total
                homeward(k).start()

    @pl.loop(0, n)
    def _(k):
        over(k, t).wait_send()
        pair_own(k, t).wait_send()
        pair_far(k, across).wait_send()
        part_near(k).wait_send()
        part_far(k).wait_send()
        sum_over(k).wait_send()

        @pl.when(k > 0)
        def _():
            outward(k).wait_send()
            homeward(k).wait_send()
            homeward(k).wait_recv()


def run_experts(outgoing, gate_weight, up_weight, down_weight):
    n, cap, width = outgoing.shape
    tp = lax.axis_size("tp")
    units = gate_weight.shape[1]
    vmem = pl.BlockSpec(memory_space=pltpu.VMEM)
    hbm = pl.BlockSpec(memory_space=pl.ANY)
    bf16 = jnp.bfloat16
    return pl.pallas_call(
        functools.partial(expert_kernel, n, tp),
        out_shape=jax.ShapeDtypeStruct((n, cap, width), bf16),
        in_specs=[vmem, hbm, hbm, hbm],
        out_specs=vmem,
        scratch_shapes=[
            pltpu.VMEM((n, tp, cap, width), bf16),
            pltpu.VMEM((n, tp, cap, width), bf16),
            pltpu.VMEM((n, 2, cap, width), bf16),
            pltpu.VMEM((n, cap, width), bf16),
            pltpu.VMEM((n, cap, width), bf16),
            pltpu.VMEM((n, cap, width), bf16),
            pltpu.VMEM(gate_weight.shape, bf16),
            pltpu.VMEM(up_weight.shape, bf16),
            pltpu.VMEM(down_weight.shape, bf16),
            pltpu.VMEM((tp * cap, units), bf16),
            pltpu.SemaphoreType.DMA((4,)),
            pltpu.SemaphoreType.DMA((8, n)),
            pltpu.SemaphoreType.DMA((8, n)),
        ],
        compiler_params=pltpu.CompilerParams(
            collective_id=1, has_side_effects=True, vmem_limit_bytes=60 * 1024 * 1024
        ),
    )(outgoing, gate_weight, up_weight, down_weight)


def body(
    gate_in,
    value_in,
    gate_out,
    conv_taps,
    proj_weight,
    residual,
    norm_gain,
    routes,
    route_weight,
    expert_gate,
    expert_up,
    expert_down,
):
    tok_dev = gate_in.shape[0]
    model_width = residual.shape[1]
    tp_count = lax.axis_size("tp")
    groups = lax.axis_size("sp")
    quarter = residual.shape[0]
    top_count = routes.shape[1]
    capacity = 2 * quarter * top_count // groups
    tp_index = lax.axis_index("tp")
    first_own = tp_index * quarter
    prior_gate, prior_value = passed_along(
        (gate_in[tok_dev - 2 :], value_in[tok_dev - 2 :]), "sp", 1
    )
    product = gate_in.astype(jnp.float32) * value_in.astype(jnp.float32)
    prior_mix = prior_gate.astype(jnp.float32) * prior_value.astype(jnp.float32)
    padded = jnp.concatenate([prior_mix, product], axis=0)
    conv_sum = conv_taps[0] * padded[:-2] + conv_taps[1] * padded[1:-1] + conv_taps[2] * padded[2:]
    mixed_out = (gate_out.astype(jnp.float32) * conv_sum).astype(jnp.bfloat16)
    own_routes = lax.dynamic_slice_in_dim(routes, first_own, quarter, 0)
    own_weights = lax.dynamic_slice_in_dim(route_weight, first_own, quarter, 0)
    row_block = mixed_out
    summed = lax.psum_scatter(
        rounded(jnp.dot(row_block, proj_weight, preferred_element_type=jnp.float32)).astype(
            jnp.bfloat16
        ),
        "tp",
        scatter_dimension=0,
        tiled=True,
    ).astype(jnp.float32)
    my_rows = residual.astype(jnp.float32) + summed
    normed = normalize(my_rows, norm_gain)
    own_slots = slot_numbers(own_routes, quarter, groups)
    flat_pick = own_routes * capacity + own_slots
    slot_count = groups * capacity
    outgoing = dispatch_rows(normed, flat_pick, slot_count)
    returned = run_experts(
        outgoing.reshape(groups, capacity, model_width),
        expert_gate[0],
        expert_up[0],
        expert_down[0],
    ).reshape(slot_count, model_width)
    total = my_rows
    for k in range(top_count):
        pick = flat_pick[:, k, None] == jnp.arange(slot_count, dtype=jnp.int32)
        picked = jnp.dot(
            pick.astype(jnp.bfloat16), returned, preferred_element_type=jnp.float32
        )
        total = total + own_weights[:, k, None] * picked
    return total.astype(jnp.bfloat16)


def solution(mesh):
    placed = (
        P("sp", "tp"),
        P("sp", "tp"),
        P("sp", "tp"),
        P(None, "tp"),
        P("tp", None),
        P(("sp", "tp"), None),
        P(),
        P("sp", None),
        P("sp", None),
        P("sp", None, "tp"),
        P("sp", None, "tp"),
        P("sp", "tp", None),
    )
    return jax.shard_map(
        body, mesh=mesh, in_specs=placed, out_specs=P(("sp", "tp"), None), check_vma=False
    )
```

```python
import functools

import jax
import jax.numpy as jnp
from jax import lax
from jax.experimental import pallas as pl
from jax.experimental.pallas import tpu as pltpu
from jax.sharding import PartitionSpec as P


def slot_numbers(route_ids, block_rows, expert_count):
    block_count = route_ids.shape[0] // block_rows
    flat_ids = route_ids.reshape(block_count, block_rows * route_ids.shape[1])
    one_hot = (
        flat_ids[:, :, None] == jnp.arange(expert_count, dtype=jnp.int32)[None, None, :]
    ).astype(jnp.int32)
    before = jnp.cumsum(one_hot, axis=1) - one_hot
    return jnp.sum(before * one_hot, axis=2).reshape(route_ids.shape)


def dispatch_rows(normed, flat_pick, slot_count):
    slot_ids = jnp.arange(slot_count, dtype=jnp.int32)
    chosen = jnp.any(flat_pick[None, :, :] == slot_ids[:, None, None], axis=2)
    return jnp.dot(
        chosen.astype(jnp.bfloat16), normed, preferred_element_type=jnp.float32
    ).astype(jnp.bfloat16)


MESH = pl.DeviceIdType.MESH


def mixer_kernel(
    n, tp, halo, pieces, gate_ref, value_ref, out_gate_ref, taps_ref, proj_ref, res_ref, gain_ref,
    rows_ref, normed_ref, edge, product, mixed, part, mrecv, psum, xrecv, send, got,
):
    s = lax.axis_index("sp")
    t = lax.axis_index("tp")
    mate = t + 1 - 2 * (t % 2)
    across = (t + 2) % tp
    mate_across = (mate + 2) % tp
    tokens = gate_ref.shape[0]
    quarter, width = res_ref.shape
    piece = quarter // pieces
    after, before = (s + 1) % n, (s + n - 1) % n

    barrier = pltpu.get_barrier_semaphore()
    for peer in ((s, mate), (s, across), (after, t), (before, t)):
        pl.semaphore_signal(barrier, inc=1, device_id=peer, device_id_type=MESH)

    def remote(src, dst, lane, device):
        return pltpu.make_async_remote_copy(
            src_ref=src,
            dst_ref=dst,
            send_sem=send.at[lane],
            recv_sem=got.at[lane],
            device_id=device,
            device_id_type=MESH,
        )

    tail = pl.ds(tokens - halo, halo)
    edges = [
        remote(ref.at[tail], edge.at[i], i, (after, t))
        for i, ref in enumerate((gate_ref, value_ref))
    ]
    pl.semaphore_wait(barrier, 4)
    for copy in edges:
        copy.start()

    body_rows = pl.ds(halo, tokens)
    product[body_rows] = gate_ref[...].astype(jnp.float32) * value_ref[...].astype(jnp.float32)
    for copy in edges:
        copy.wait_recv()
    prior = edge[0].astype(jnp.float32) * edge[1].astype(jnp.float32)
    product[pl.ds(0, halo)] = jnp.where(s == 0, 0.0, prior)
    conv_sum = (
        taps_ref[0:1] * product[pl.ds(halo - 2, tokens)]
        + taps_ref[1:2] * product[pl.ds(halo - 1, tokens)]
        + taps_ref[2:3] * product[body_rows]
    )
    mixed[...] = (out_gate_ref[...].astype(jnp.float32) * conv_sum).astype(jnp.bfloat16)

    def project(block, p):
        first = pl.multiple_of(block * quarter + p * piece, piece)
        y = jnp.dot(
            mixed[pl.ds(first, piece)], proj_ref[...], preferred_element_type=jnp.float32
        )
        part[block, p] = y.astype(jnp.bfloat16)

    def lane(kind, p):
        return 2 + kind * pieces + p

    def to_mate(kind, block, p):
        return remote(part.at[block, p], mrecv.at[kind, p], lane(kind, p), (s, mate))

    def over(p):
        return remote(psum.at[p], xrecv.at[p], lane(2, p), (s, across))

    def wide(block):
        return block.astype(jnp.float32)

    for p in range(pieces):
        project(mate_across, p)
        to_mate(0, mate_across, p).start()
    for p in range(pieces):
        project(across, p)
        to_mate(0, mate_across, p).wait_recv()
        psum[p] = (wide(part[across, p]) + wide(mrecv[0, p])).astype(jnp.bfloat16)
        over(p).start()
    for p in range(pieces):
        project(mate, p)
        to_mate(1, mate, p).start()
    for p in range(pieces):
        project(t, p)
    for p in range(pieces):
        to_mate(1, mate, p).wait_recv()
        over(p).wait_recv()
        at = pl.ds(p * piece, piece)
        summed = wide(part[t, p]) + wide(mrecv[1, p]) + wide(xrecv[p])
        hidden_rows = wide(res_ref[at]) + summed
        inverse = lax.rsqrt(jnp.mean(hidden_rows * hidden_rows, axis=-1, keepdims=True) + 1e-05)
        rows_ref[at] = hidden_rows
        normed_ref[at] = (hidden_rows * inverse * gain_ref[...]).astype(jnp.bfloat16)
    for copy in edges:
        copy.wait_send()
    for p in range(pieces):
        to_mate(0, mate_across, p).wait_send()
        to_mate(1, mate, p).wait_send()
        over(p).wait_send()


def run_mixer(gate_in, value_in, gate_out, conv_taps, proj_weight, residual, norm_gain):
    n, tp = lax.axis_size("sp"), lax.axis_size("tp")
    tokens, channels = gate_in.shape
    quarter, width = residual.shape
    halo, pieces = 16, 4
    piece = quarter // pieces
    vmem = pl.BlockSpec(memory_space=pltpu.VMEM)
    bf16, f32 = jnp.bfloat16, jnp.float32
    return pl.pallas_call(
        functools.partial(mixer_kernel, n, tp, halo, pieces),
        out_shape=(
            jax.ShapeDtypeStruct((quarter, width), f32),
            jax.ShapeDtypeStruct((quarter, width), bf16),
        ),
        in_specs=[vmem] * 7,
        out_specs=(vmem, vmem),
        scratch_shapes=[
            pltpu.VMEM((2, halo, channels), bf16),
            pltpu.VMEM((halo + tokens, channels), f32),
            pltpu.VMEM((tokens, channels), bf16),
            pltpu.VMEM((tp, pieces, piece, width), bf16),
            pltpu.VMEM((2, pieces, piece, width), bf16),
            pltpu.VMEM((pieces, piece, width), bf16),
            pltpu.VMEM((pieces, piece, width), bf16),
            pltpu.SemaphoreType.DMA((2 + 3 * pieces,)),
            pltpu.SemaphoreType.DMA((2 + 3 * pieces,)),
        ],
        compiler_params=pltpu.CompilerParams(
            collective_id=2, has_side_effects=True, vmem_limit_bytes=60 * 1024 * 1024
        ),
    )(gate_in, value_in, gate_out, conv_taps, proj_weight, residual, norm_gain.reshape(1, width))


def expert_kernel(
    n, tp, out_ref, gate_hbm, up_hbm, down_hbm, ret_ref,
    recv, part, mrecv, psum, xrecv, fin, gate_w, up_w, down_w, hid, local_sem, send, got,
):
    s = lax.axis_index("sp")
    t = lax.axis_index("tp")
    mate = t + 1 - 2 * (t % 2)
    across = (t + 2) % tp
    mate_across = (mate + 2) % tp
    cap, width = out_ref.shape[1], out_ref.shape[2]
    units = gate_w.shape[1]
    rows = tp * cap

    weight_copies = [
        pltpu.make_async_copy(src, dst, local_sem.at[i])
        for i, (src, dst) in enumerate(
            [(gate_hbm, gate_w), (up_hbm, up_w), (down_hbm, down_w)]
        )
    ]
    for copy in weight_copies:
        copy.start()

    barrier = pltpu.get_barrier_semaphore()

    @pl.loop(1, n)
    def _(k):
        pl.semaphore_signal(barrier, inc=1, device_id=((s + k) % n, t), device_id_type=MESH)

    for peer in (mate, across):
        pl.semaphore_signal(barrier, inc=1, device_id=(s, peer), device_id_type=MESH)
    pl.semaphore_wait(barrier, n + 1)

    def remote(src, dst, lane, k, device):
        return pltpu.make_async_remote_copy(
            src_ref=src,
            dst_ref=dst,
            send_sem=send.at[lane, k],
            recv_sem=got.at[lane, k],
            device_id=device,
            device_id_type=MESH,
        )

    def outward(k):
        to = (s + k) % n
        return remote(out_ref.at[to], recv.at[k, t], 0, k, (to, t))

    def over(k, block):
        return remote(recv.at[k, block], recv.at[k, block], 1, k, (s, across))

    def pair_own(k, block):
        return remote(recv.at[k, block], recv.at[k, block], 2, k, (s, mate))

    def pair_far(k, block):
        return remote(recv.at[k, block], recv.at[k, block], 3, k, (s, mate))

    def part_near(k):
        return remote(part.at[k, mate], mrecv.at[k, 0], 4, k, (s, mate))

    def part_far(k):
        return remote(part.at[k, mate_across], mrecv.at[k, 1], 5, k, (s, mate))

    def sum_over(k):
        return remote(psum.at[k], xrecv.at[k], 6, k, (s, across))

    def homeward(k):
        return remote(fin.at[k], ret_ref.at[s], 7, k, ((s + n - k) % n, t))

    own = pltpu.make_async_copy(out_ref.at[s], recv.at[0, t], local_sem.at[3])
    own.start()

    @pl.loop(1, n)
    def _(k):
        outward(k).start()

    own.wait()

    def ffn(k):
        def load():
            block = recv[k]
            if cap % 16:
                return block.astype(jnp.float32).reshape(rows, width).astype(jnp.bfloat16)
            return block.reshape(rows, width)

        cols = min(256, units)

        @pl.loop(0, units // cols)
        def _(c):
            at = pl.ds(pl.multiple_of(c * cols, cols), cols)
            x = load()
            gate = jnp.dot(x, gate_w[:, at], preferred_element_type=jnp.float32)
            up = jnp.dot(x, up_w[:, at], preferred_element_type=jnp.float32)
            hid[:, at] = (gate / (1.0 + jnp.exp(-gate)) * up).astype(jnp.bfloat16)

        wide = min(512, width)

        @pl.loop(0, width // wide)
        def _(c):
            at = pl.ds(pl.multiple_of(c * wide, wide), wide)
            y = jnp.dot(hid[...], down_w[:, at], preferred_element_type=jnp.float32)
            part[k, :, :, at] = y.reshape(tp, cap, wide).astype(jnp.bfloat16)

    def wide_sum(*blocks):
        total = blocks[0].astype(jnp.float32)
        for block in blocks[1:]:
            total = total + block.astype(jnp.float32)
        return total

    @pl.loop(0, n + 4)
    def _(i):
        @pl.when(i < n)
        def _():
            @pl.when(i > 0)
            def _():
                outward(i).wait_recv()

            over(i, t).start()
            pair_own(i, t).start()

        @pl.when((i >= 1) & (i < n + 1))
        def _():
            k = i - 1
            over(k, across).wait_recv()
            pair_far(k, across).start()

        @pl.when(i == 2)
        def _():
            for copy in weight_copies:
                copy.wait()

        @pl.when((i >= 2) & (i < n + 2))
        def _():
            k = i - 2
            pair_own(k, mate).wait_recv()
            pair_far(k, mate_across).wait_recv()
            ffn(k)
            part_far(k).start()
            part_near(k).start()

        @pl.when((i >= 3) & (i < n + 3))
        def _():
            k = i - 3
            part_far(k).wait_recv()
            psum[k] = wide_sum(part[k, across], mrecv[k, 1]).astype(jnp.bfloat16)
            sum_over(k).start()

        @pl.when(i >= 4)
        def _():
            k = i - 4
            part_near(k).wait_recv()
            sum_over(k).wait_recv()
            total = wide_sum(part[k, t], mrecv[k, 0], xrecv[k]).astype(jnp.bfloat16)

            @pl.when(k == 0)
            def _():
                ret_ref[s] = total

            @pl.when(k > 0)
            def _():
                fin[k] = total
                homeward(k).start()

    @pl.loop(0, n)
    def _(k):
        over(k, t).wait_send()
        pair_own(k, t).wait_send()
        pair_far(k, across).wait_send()
        part_near(k).wait_send()
        part_far(k).wait_send()
        sum_over(k).wait_send()

        @pl.when(k > 0)
        def _():
            outward(k).wait_send()
            homeward(k).wait_send()
            homeward(k).wait_recv()


def run_experts(outgoing, gate_weight, up_weight, down_weight):
    n, cap, width = outgoing.shape
    tp = lax.axis_size("tp")
    units = gate_weight.shape[1]
    vmem = pl.BlockSpec(memory_space=pltpu.VMEM)
    hbm = pl.BlockSpec(memory_space=pl.ANY)
    bf16 = jnp.bfloat16
    return pl.pallas_call(
        functools.partial(expert_kernel, n, tp),
        out_shape=jax.ShapeDtypeStruct((n, cap, width), bf16),
        in_specs=[vmem, hbm, hbm, hbm],
        out_specs=vmem,
        scratch_shapes=[
            pltpu.VMEM((n, tp, cap, width), bf16),
            pltpu.VMEM((n, tp, cap, width), bf16),
            pltpu.VMEM((n, 2, cap, width), bf16),
            pltpu.VMEM((n, cap, width), bf16),
            pltpu.VMEM((n, cap, width), bf16),
            pltpu.VMEM((n, cap, width), bf16),
            pltpu.VMEM(gate_weight.shape, bf16),
            pltpu.VMEM(up_weight.shape, bf16),
            pltpu.VMEM(down_weight.shape, bf16),
            pltpu.VMEM((tp * cap, units), bf16),
            pltpu.SemaphoreType.DMA((4,)),
            pltpu.SemaphoreType.DMA((8, n)),
            pltpu.SemaphoreType.DMA((8, n)),
        ],
        compiler_params=pltpu.CompilerParams(
            collective_id=1, has_side_effects=True, vmem_limit_bytes=60 * 1024 * 1024
        ),
    )(outgoing, gate_weight, up_weight, down_weight)


def body(
    gate_in,
    value_in,
    gate_out,
    conv_taps,
    proj_weight,
    residual,
    norm_gain,
    routes,
    route_weight,
    expert_gate,
    expert_up,
    expert_down,
):
    model_width = residual.shape[1]
    tp_count = lax.axis_size("tp")
    groups = lax.axis_size("sp")
    quarter = residual.shape[0]
    top_count = routes.shape[1]
    capacity = 2 * quarter * top_count // groups
    tp_index = lax.axis_index("tp")
    first_own = tp_index * quarter
    own_routes = lax.dynamic_slice_in_dim(routes, first_own, quarter, 0)
    own_weights = lax.dynamic_slice_in_dim(route_weight, first_own, quarter, 0)
    my_rows, normed = run_mixer(
        gate_in, value_in, gate_out, conv_taps, proj_weight, residual, norm_gain
    )
    own_slots = slot_numbers(own_routes, quarter, groups)
    flat_pick = own_routes * capacity + own_slots
    slot_count = groups * capacity
    outgoing = dispatch_rows(normed, flat_pick, slot_count)
    returned = run_experts(
        outgoing.reshape(groups, capacity, model_width),
        expert_gate[0],
        expert_up[0],
        expert_down[0],
    ).reshape(slot_count, model_width)
    total = my_rows
    for k in range(top_count):
        pick = flat_pick[:, k, None] == jnp.arange(slot_count, dtype=jnp.int32)
        picked = jnp.dot(
            pick.astype(jnp.bfloat16), returned, preferred_element_type=jnp.float32
        )
        total = total + own_weights[:, k, None] * picked
    return total.astype(jnp.bfloat16)


def solution(mesh):
    placed = (
        P("sp", "tp"),
        P("sp", "tp"),
        P("sp", "tp"),
        P(None, "tp"),
        P("tp", None),
        P(("sp", "tp"), None),
        P(),
        P("sp", None),
        P("sp", None),
        P("sp", None, "tp"),
        P("sp", None, "tp"),
        P("sp", "tp", None),
    )
    return jax.shard_map(
        body, mesh=mesh, in_specs=placed, out_specs=P(("sp", "tp"), None), check_vma=False
    )
```

```python
import functools

import jax
import jax.numpy as jnp
from jax import lax
from jax.experimental import pallas as pl
from jax.experimental.pallas import tpu as pltpu
from jax.sharding import PartitionSpec as P


def slot_numbers(route_ids, block_rows, expert_count):
    block_count = route_ids.shape[0] // block_rows
    flat_ids = route_ids.reshape(block_count, block_rows * route_ids.shape[1])
    one_hot = (
        flat_ids[:, :, None] == jnp.arange(expert_count, dtype=jnp.int32)[None, None, :]
    ).astype(jnp.int32)
    before = jnp.cumsum(one_hot, axis=1) - one_hot
    return jnp.sum(before * one_hot, axis=2).reshape(route_ids.shape)


def dispatch_rows(normed, flat_pick, slot_count):
    slot_ids = jnp.arange(slot_count, dtype=jnp.int32)
    chosen = jnp.any(flat_pick[None, :, :] == slot_ids[:, None, None], axis=2)
    return jnp.dot(
        chosen.astype(jnp.bfloat16), normed, preferred_element_type=jnp.float32
    ).astype(jnp.bfloat16)


MESH = pl.DeviceIdType.MESH


def mixer_kernel(
    n, tp, halo, pieces, gate_ref, value_ref, out_gate_ref, taps_ref, proj_ref, res_ref, gain_ref,
    rows_ref, normed_ref, edge, product, mixed, part, mrecv, psum, xrecv, send, got,
):
    s = lax.axis_index("sp")
    t = lax.axis_index("tp")
    mate = t + 1 - 2 * (t % 2)
    across = (t + 2) % tp
    mate_across = (mate + 2) % tp
    tokens = gate_ref.shape[0]
    quarter, width = res_ref.shape
    piece = quarter // pieces
    after, before = (s + 1) % n, (s + n - 1) % n

    barrier = pltpu.get_barrier_semaphore()
    for peer in ((s, mate), (s, across), (after, t), (before, t)):
        pl.semaphore_signal(barrier, inc=1, device_id=peer, device_id_type=MESH)

    def remote(src, dst, lane, device):
        return pltpu.make_async_remote_copy(
            src_ref=src,
            dst_ref=dst,
            send_sem=send.at[lane],
            recv_sem=got.at[lane],
            device_id=device,
            device_id_type=MESH,
        )

    tail = pl.ds(tokens - halo, halo)
    edges = [
        remote(ref.at[tail], edge.at[i], i, (after, t))
        for i, ref in enumerate((gate_ref, value_ref))
    ]
    pl.semaphore_wait(barrier, 4)
    for copy in edges:
        copy.start()

    body_rows = pl.ds(halo, tokens)
    product[body_rows] = gate_ref[...].astype(jnp.float32) * value_ref[...].astype(jnp.float32)
    for copy in edges:
        copy.wait_recv()
    prior = edge[0].astype(jnp.float32) * edge[1].astype(jnp.float32)
    product[pl.ds(0, halo)] = jnp.where(s == 0, 0.0, prior)
    conv_sum = (
        taps_ref[0:1] * product[pl.ds(halo - 2, tokens)]
        + taps_ref[1:2] * product[pl.ds(halo - 1, tokens)]
        + taps_ref[2:3] * product[body_rows]
    )
    mixed[...] = (out_gate_ref[...].astype(jnp.float32) * conv_sum).astype(jnp.bfloat16)

    def project(block, p):
        first = pl.multiple_of(block * quarter + p * piece, piece)
        y = jnp.dot(
            mixed[pl.ds(first, piece)], proj_ref[...], preferred_element_type=jnp.float32
        )
        part[block, p] = y.astype(jnp.bfloat16)

    def lane(kind, p):
        return 2 + kind * pieces + p

    def to_mate(kind, block, p):
        return remote(part.at[block, p], mrecv.at[kind, p], lane(kind, p), (s, mate))

    def over(p):
        return remote(psum.at[p], xrecv.at[p], lane(2, p), (s, across))

    def wide(block):
        return block.astype(jnp.float32)

    for p in range(pieces):
        project(mate_across, p)
        to_mate(0, mate_across, p).start()
    for p in range(pieces):
        project(across, p)
        to_mate(0, mate_across, p).wait_recv()
        psum[p] = (wide(part[across, p]) + wide(mrecv[0, p])).astype(jnp.bfloat16)
        over(p).start()
    for p in range(pieces):
        project(mate, p)
        to_mate(1, mate, p).start()
    for p in range(pieces):
        project(t, p)
    for p in range(pieces):
        to_mate(1, mate, p).wait_recv()
        over(p).wait_recv()
        at = pl.ds(p * piece, piece)
        summed = wide(part[t, p]) + wide(mrecv[1, p]) + wide(xrecv[p])
        hidden_rows = wide(res_ref[at]) + summed
        inverse = lax.rsqrt(jnp.mean(hidden_rows * hidden_rows, axis=-1, keepdims=True) + 1e-05)
        rows_ref[at] = hidden_rows
        normed_ref[at] = (hidden_rows * inverse * gain_ref[...]).astype(jnp.bfloat16)
    for copy in edges:
        copy.wait_send()
    for p in range(pieces):
        to_mate(0, mate_across, p).wait_send()
        to_mate(1, mate, p).wait_send()
        over(p).wait_send()


def run_mixer(gate_in, value_in, gate_out, conv_taps, proj_weight, residual, norm_gain):
    n, tp = lax.axis_size("sp"), lax.axis_size("tp")
    tokens, channels = gate_in.shape
    quarter, width = residual.shape
    halo, pieces = 16, 4
    piece = quarter // pieces
    vmem = pl.BlockSpec(memory_space=pltpu.VMEM)
    bf16, f32 = jnp.bfloat16, jnp.float32
    return pl.pallas_call(
        functools.partial(mixer_kernel, n, tp, halo, pieces),
        out_shape=(
            jax.ShapeDtypeStruct((quarter, width), f32),
            jax.ShapeDtypeStruct((quarter, width), bf16),
        ),
        in_specs=[vmem] * 7,
        out_specs=(vmem, vmem),
        scratch_shapes=[
            pltpu.VMEM((2, halo, channels), bf16),
            pltpu.VMEM((halo + tokens, channels), f32),
            pltpu.VMEM((tokens, channels), bf16),
            pltpu.VMEM((tp, pieces, piece, width), bf16),
            pltpu.VMEM((2, pieces, piece, width), bf16),
            pltpu.VMEM((pieces, piece, width), bf16),
            pltpu.VMEM((pieces, piece, width), bf16),
            pltpu.SemaphoreType.DMA((2 + 3 * pieces,)),
            pltpu.SemaphoreType.DMA((2 + 3 * pieces,)),
        ],
        compiler_params=pltpu.CompilerParams(
            collective_id=2, has_side_effects=True, vmem_limit_bytes=60 * 1024 * 1024
        ),
    )(gate_in, value_in, gate_out, conv_taps, proj_weight, residual, norm_gain.reshape(1, width))


def expert_kernel(
    n, tp, halves, out_ref, gate_hbm, up_hbm, down_hbm, ret_ref,
    recv, part, mrecv, psum, xrecv, fin, gate_w, up_w, down_w, hid, local_sem, send, got,
):
    s = lax.axis_index("sp")
    t = lax.axis_index("tp")
    mate = t + 1 - 2 * (t % 2)
    across = (t + 2) % tp
    mate_across = (mate + 2) % tp
    cap, width = out_ref.shape[1], out_ref.shape[2]
    units = gate_w.shape[1]
    rows = tp * cap
    steps = n * halves

    weight_copies = [
        pltpu.make_async_copy(src, dst, local_sem.at[i])
        for i, (src, dst) in enumerate(
            [(gate_hbm, gate_w), (up_hbm, up_w), (down_hbm, down_w)]
        )
    ]
    for copy in weight_copies:
        copy.start()

    barrier = pltpu.get_barrier_semaphore()

    @pl.loop(1, n)
    def _(k):
        pl.semaphore_signal(barrier, inc=1, device_id=((s + k) % n, t), device_id_type=MESH)

    for peer in (mate, across):
        pl.semaphore_signal(barrier, inc=1, device_id=(s, peer), device_id_type=MESH)
    pl.semaphore_wait(barrier, n + 1)

    def remote(src, dst, lane, k, device):
        return pltpu.make_async_remote_copy(
            src_ref=src,
            dst_ref=dst,
            send_sem=send.at[lane, k],
            recv_sem=got.at[lane, k],
            device_id=device,
            device_id_type=MESH,
        )

    def outward(k):
        to = (s + k // halves) % n
        return remote(out_ref.at[to * halves + k % halves], recv.at[k, t], 0, k, (to, t))

    def over(k, block):
        return remote(recv.at[k, block], recv.at[k, block], 1, k, (s, across))

    def pair_own(k, block):
        return remote(recv.at[k, block], recv.at[k, block], 2, k, (s, mate))

    def pair_far(k, block):
        return remote(recv.at[k, block], recv.at[k, block], 3, k, (s, mate))

    def part_near(k):
        return remote(part.at[k, mate], mrecv.at[k, 0], 4, k, (s, mate))

    def part_far(k):
        return remote(part.at[k, mate_across], mrecv.at[k, 1], 5, k, (s, mate))

    def sum_over(k):
        return remote(psum.at[k], xrecv.at[k], 6, k, (s, across))

    def homeward(k):
        to = (s + n - k // halves) % n
        return remote(fin.at[k], ret_ref.at[s * halves + k % halves], 7, k, (to, t))

    own = [
        pltpu.make_async_copy(out_ref.at[s * halves + h], recv.at[h, t], local_sem.at[3 + h])
        for h in range(halves)
    ]
    for copy in own:
        copy.start()

    @pl.loop(halves, steps)
    def _(k):
        outward(k).start()

    for copy in own:
        copy.wait()

    def ffn(k):
        def load():
            block = recv[k]
            if cap % 16:
                return block.astype(jnp.float32).reshape(rows, width).astype(jnp.bfloat16)
            return block.reshape(rows, width)

        cols = min(256, units)

        @pl.loop(0, units // cols)
        def _(c):
            at = pl.ds(pl.multiple_of(c * cols, cols), cols)
            x = load()
            gate = jnp.dot(x, gate_w[:, at], preferred_element_type=jnp.float32)
            up = jnp.dot(x, up_w[:, at], preferred_element_type=jnp.float32)
            hid[:, at] = (gate / (1.0 + jnp.exp(-gate)) * up).astype(jnp.bfloat16)

        wide = min(512, width)

        @pl.loop(0, width // wide)
        def _(c):
            at = pl.ds(pl.multiple_of(c * wide, wide), wide)
            y = jnp.dot(hid[...], down_w[:, at], preferred_element_type=jnp.float32)
            part[k, :, :, at] = y.reshape(tp, cap, wide).astype(jnp.bfloat16)

    def wide_sum(*blocks):
        total = blocks[0].astype(jnp.float32)
        for block in blocks[1:]:
            total = total + block.astype(jnp.float32)
        return total

    @pl.loop(0, steps + 4)
    def _(i):
        @pl.when(i < steps)
        def _():
            @pl.when(i >= halves)
            def _():
                outward(i).wait_recv()

            over(i, t).start()
            pair_own(i, t).start()

        @pl.when((i >= 1) & (i < steps + 1))
        def _():
            k = i - 1
            over(k, across).wait_recv()
            pair_far(k, across).start()

        @pl.when((i >= 3) & (i < steps + 3))
        def _():
            k = i - 3
            part_far(k).wait_recv()
            psum[k] = wide_sum(part[k, across], mrecv[k, 1]).astype(jnp.bfloat16)
            sum_over(k).start()

        @pl.when(i >= 4)
        def _():
            k = i - 4
            part_near(k).wait_recv()
            sum_over(k).wait_recv()
            total = wide_sum(part[k, t], mrecv[k, 0], xrecv[k]).astype(jnp.bfloat16)

            @pl.when(k < halves)
            def _():
                ret_ref[s * halves + k] = total

            @pl.when(k >= halves)
            def _():
                fin[k] = total
                homeward(k).start()

        @pl.when(i == 2)
        def _():
            for copy in weight_copies:
                copy.wait()

        @pl.when((i >= 2) & (i < steps + 2))
        def _():
            k = i - 2
            pair_own(k, mate).wait_recv()
            pair_far(k, mate_across).wait_recv()
            ffn(k)
            part_far(k).start()
            part_near(k).start()

    @pl.loop(0, steps)
    def _(k):
        over(k, t).wait_send()
        pair_own(k, t).wait_send()
        pair_far(k, across).wait_send()
        part_near(k).wait_send()
        part_far(k).wait_send()
        sum_over(k).wait_send()

        @pl.when(k >= halves)
        def _():
            outward(k).wait_send()
            homeward(k).wait_send()
            homeward(k).wait_recv()


def run_experts(outgoing, gate_weight, up_weight, down_weight):
    n, cap, width = outgoing.shape
    tp = lax.axis_size("tp")
    units = gate_weight.shape[1]
    halves = 2 if cap % 32 == 0 else 1
    steps, cap = n * halves, cap // halves
    vmem = pl.BlockSpec(memory_space=pltpu.VMEM)
    hbm = pl.BlockSpec(memory_space=pl.ANY)
    bf16 = jnp.bfloat16
    return pl.pallas_call(
        functools.partial(expert_kernel, n, tp, halves),
        out_shape=jax.ShapeDtypeStruct((steps, cap, width), bf16),
        in_specs=[vmem, hbm, hbm, hbm],
        out_specs=vmem,
        scratch_shapes=[
            pltpu.VMEM((steps, tp, cap, width), bf16),
            pltpu.VMEM((steps, tp, cap, width), bf16),
            pltpu.VMEM((steps, 2, cap, width), bf16),
            pltpu.VMEM((steps, cap, width), bf16),
            pltpu.VMEM((steps, cap, width), bf16),
            pltpu.VMEM((steps, cap, width), bf16),
            pltpu.VMEM(gate_weight.shape, bf16),
            pltpu.VMEM(up_weight.shape, bf16),
            pltpu.VMEM(down_weight.shape, bf16),
            pltpu.VMEM((tp * cap, units), bf16),
            pltpu.SemaphoreType.DMA((3 + halves,)),
            pltpu.SemaphoreType.DMA((8, steps)),
            pltpu.SemaphoreType.DMA((8, steps)),
        ],
        compiler_params=pltpu.CompilerParams(
            collective_id=1, has_side_effects=True, vmem_limit_bytes=60 * 1024 * 1024
        ),
    )(outgoing.reshape(steps, cap, width), gate_weight, up_weight, down_weight)


def body(
    gate_in,
    value_in,
    gate_out,
    conv_taps,
    proj_weight,
    residual,
    norm_gain,
    routes,
    route_weight,
    expert_gate,
    expert_up,
    expert_down,
):
    model_width = residual.shape[1]
    tp_count = lax.axis_size("tp")
    groups = lax.axis_size("sp")
    quarter = residual.shape[0]
    top_count = routes.shape[1]
    capacity = 2 * quarter * top_count // groups
    tp_index = lax.axis_index("tp")
    first_own = tp_index * quarter
    own_routes = lax.dynamic_slice_in_dim(routes, first_own, quarter, 0)
    own_weights = lax.dynamic_slice_in_dim(route_weight, first_own, quarter, 0)
    my_rows, normed = run_mixer(
        gate_in, value_in, gate_out, conv_taps, proj_weight, residual, norm_gain
    )
    own_slots = slot_numbers(own_routes, quarter, groups)
    flat_pick = own_routes * capacity + own_slots
    slot_count = groups * capacity
    outgoing = dispatch_rows(normed, flat_pick, slot_count)
    returned = run_experts(
        outgoing.reshape(groups, capacity, model_width),
        expert_gate[0],
        expert_up[0],
        expert_down[0],
    ).reshape(slot_count, model_width)
    total = my_rows
    for k in range(top_count):
        pick = flat_pick[:, k, None] == jnp.arange(slot_count, dtype=jnp.int32)
        picked = jnp.dot(
            pick.astype(jnp.bfloat16), returned, preferred_element_type=jnp.float32
        )
        total = total + own_weights[:, k, None] * picked
    return total.astype(jnp.bfloat16)


def solution(mesh):
    placed = (
        P("sp", "tp"),
        P("sp", "tp"),
        P("sp", "tp"),
        P(None, "tp"),
        P("tp", None),
        P(("sp", "tp"), None),
        P(),
        P("sp", None),
        P("sp", None),
        P("sp", None, "tp"),
        P("sp", None, "tp"),
        P("sp", "tp", None),
    )
    return jax.shard_map(
        body, mesh=mesh, in_specs=placed, out_specs=P(("sp", "tp"), None), check_vma=False
    )
```
